32 devices in a mesh: ep: 32 (over z, y, x, core).
Axes of the slice: x: 2, y: 2, z: 4, core: 2. Of those that a mesh axis runs over, the one named last changes fastest.
Arguments:
- tokens: bfloat16 [1024, 3072], P('ep'), may hold values from -6 to 6
- norm_gain: float32 [3072], replicated, may hold values from 0.1 to 1.9
- expert_ids: int32 [1024, 4], P('ep'), may hold values from 0 to 31, as said below
- expert_scores: float32 [1024, 4], P('ep'), may hold values from -100 to 180
- group_prob: float32 [1024], P('ep'), may hold values from 0.25 to 1
- gate_weight: bfloat16 [32, 3072, 384], P('ep'), may hold values from -0.109375 to 0.109375
- up_weight: bfloat16 [32, 3072, 384], P('ep'), may hold values from -0.109375 to 0.109375
- down_weight: bfloat16 [32, 384, 3072], P('ep'), may hold values from -0.3125 to 0.3125
Outputs:
- combined: bfloat16 [1024, 3072], P('ep')
The draws below stay inside these ranges and needn't reach their ends.
Inputs may be any that keep to these rules, and one draw needn't show every extreme that they name: `expert_ids`: the 4 ids of a row are different and lie in one group of 8 consecutive experts. Among the rows of one device no expert is named by more than 16 rows, and in every draw some expert is named by exactly 16 rows of one device.
All inputs are finite; a program needn't handle non-finite values.
Results may differ from the reference program's by a relative error of at most 0.0085.
Values may be sent and summed in bfloat16 or wider, within the bound.
A program may use at most 128 MiB of HBM per device.

```python
import jax
import jax.numpy as jnp
from jax import lax

D = 3072
FFE = 384
GROUPS = 4
TOP_K = 4
TOK_DEV = 32
EXPERTS = 32
TOKENS = 1024
MOST = 16
N_EP = 32


def draw_expert_ids(key, part):
    blocks_count = TOKENS // TOK_DEV
    group_size = EXPERTS // GROUPS
    hot_count = (MOST - 1) * group_size // TOP_K + 1
    keys = jax.random.split(jax.random.fold_in(key, 11), 5)
    group_order = jax.random.permutation(keys[0], GROUPS)
    chosen_rank = jnp.min(jax.random.randint(keys[1], (3, blocks_count, TOK_DEV), 0, GROUPS), axis=0)
    hot_rank = jnp.min(jax.random.randint(keys[2], (3, blocks_count, 1), 0, GROUPS), axis=0)
    position = jnp.arange(TOK_DEV)[None, :]
    group_index = group_order[jnp.where(position < hot_count, hot_rank, chosen_rank)]
    earlier_mask = (group_index[:, :, None] == group_index[:, None, :]) & (jnp.arange(TOK_DEV)[None, None, :] < jnp.arange(TOK_DEV)[None, :, None])
    earlier = jnp.sum(earlier_mask.astype(jnp.int32), axis=2)
    starts = jax.random.randint(keys[3], (blocks_count, GROUPS), 0, group_size)
    start_here = jnp.take_along_axis(starts, group_index, axis=1)
    local_ids = (start_here[:, :, None] + earlier[:, :, None] * TOP_K + jnp.arange(TOP_K)[None, None, :]) % group_size
    global_ids = group_index[:, :, None] * group_size + local_ids
    return global_ids.reshape(TOKENS, TOP_K).astype(jnp.int32)


def draw_expert_scores(key, part):
    keys = jax.random.split(jax.random.fold_in(key, 23), 3)
    base_scores = jnp.clip(jax.random.normal(keys[0], (TOKENS, TOP_K), jnp.float32), -6.0, 6.0) * 1.5
    return base_scores.astype(jnp.float32)


def levels(rng, dims, shards, low, high):
    def one(axis_at, parts):
        heights = jax.random.uniform(jax.random.fold_in(jax.random.fold_in(rng, 6), axis_at), (parts,), jnp.float32, low / len(shards), high / len(shards))
        return jnp.repeat(jnp.exp(heights), dims[axis_at] // parts).reshape((-1,) + (1,) * (len(dims) - axis_at - 1))

    level = one(*shards[0])
    for cut in shards[1:]:
        level = level * one(*cut)
    return level


def gaussian(key, dims, deviation, reach, shards=(), kind=jnp.bfloat16):
    drawn = deviation * jax.random.normal(key, dims, jnp.float32)
    if shards:
        drawn = drawn * levels(key, dims, shards, -0.22, 0.18)
    return jnp.clip(drawn, -reach, reach).astype(kind)


def setup_inputs(seed: int = 0) -> dict:
    streams_of = jax.random.split(jax.random.key(seed), 9)
    return {
        "tokens": gaussian(streams_of[0], (TOKENS, D), 1.0, 6.0, ((0, 32),)),
        "norm_gain": jnp.clip(1.0 + 0.18 * jax.random.normal(streams_of[1], (D,), jnp.float32), 0.1, 1.9),
        "expert_ids": draw_expert_ids(jax.random.fold_in(streams_of[8], 71), 0),
        "expert_scores": draw_expert_scores(jax.random.fold_in(streams_of[8], 71), 0),
        "group_prob": jnp.clip(0.25 + 0.75 * jax.random.uniform(streams_of[4], (TOKENS,), jnp.float32) ** levels(streams_of[4], (TOKENS,), ((0, 32),), -0.2, 0.2), 0.25, 1.0),
        "gate_weight": gaussian(streams_of[5], (EXPERTS, D, FFE), D ** -0.5, 0.109375, ((0, 32),)),
        "up_weight": gaussian(streams_of[6], (EXPERTS, D, FFE), D ** -0.5, 0.109375, ((0, 32),)),
        "down_weight": gaussian(streams_of[7], (EXPERTS, FFE, D), FFE ** -0.5, 0.3125, ((0, 32),)),
    }


eps_norm = 1e-05

def layer_norm(tokens, norm_gain):
    values = tokens.astype(jnp.float32)
    average = lax.optimization_barrier(jnp.mean(values, axis=1, keepdims=True))
    centred = values - average
    variance = lax.optimization_barrier(jnp.mean(centred * centred, axis=1, keepdims=True))
    return (centred * lax.rsqrt(variance + eps_norm) * norm_gain[None, :]).astype(jnp.bfloat16)

def mixing_weights(expert_scores, group_prob):
    shifted = expert_scores - lax.optimization_barrier(jnp.max(expert_scores, axis=1, keepdims=True))
    exp_scores = jnp.exp(shifted)
    return exp_scores / lax.optimization_barrier(jnp.sum(exp_scores, axis=1, keepdims=True)) * group_prob[:, None]

def expert_rows(flat_rows, gate_matrix, up_matrix, down_matrix):
    gate_act = jnp.dot(flat_rows, gate_matrix, preferred_element_type=jnp.float32)
    up_act = jnp.dot(flat_rows, up_matrix, preferred_element_type=jnp.float32)
    hidden = (jax.nn.silu(gate_act) * up_act).astype(jnp.bfloat16)
    return jnp.dot(hidden, down_matrix, preferred_element_type=jnp.float32).astype(jnp.bfloat16)

def reference(tokens, norm_gain, expert_ids, expert_scores, group_prob, gate_weight, up_weight, down_weight):
    normed = layer_norm(tokens, norm_gain)
    weights_tok = mixing_weights(expert_scores, group_prob)
    capacity = N_EP * MOST
    slot_iota = jnp.arange(capacity, dtype=jnp.int32)

    def per_expert(running, expert_index):
        matches = expert_ids == expert_index
        chosen = jnp.any(matches, axis=1)
        own_weight = lax.optimization_barrier(jnp.sum(jnp.where(matches, weights_tok, 0.0), axis=1))
        slot_token = jnp.nonzero(chosen, size=capacity, fill_value=0)[0].astype(jnp.int32)
        filled = slot_iota < jnp.sum(chosen.astype(jnp.int32))
        results = expert_rows(normed[slot_token], gate_weight[expert_index], up_weight[expert_index], down_weight[expert_index])
        slot_scale = jnp.where(filled, own_weight[slot_token], 0.0)
        running = running.at[slot_token].add(slot_scale[:, None] * results.astype(jnp.float32))
        return (running, None)
    start = jnp.zeros((TOKENS, D), jnp.float32)
    mixture, _ = lax.scan(per_expert, start, jnp.arange(EXPERTS, dtype=jnp.int32))
    return mixture.astype(jnp.bfloat16)
```

```python
import jax
import jax.numpy as jnp
from jax import lax
from jax.sharding import PartitionSpec as P

GROUPS = 4
TOP_K = 4


eps_norm = 1e-05


def layer_norm(tokens, norm_gain):
    values = tokens.astype(jnp.float32)
    average = jnp.mean(values, axis=1, keepdims=True)
    centred = values - average
    variance = jnp.mean(centred * centred, axis=1, keepdims=True)
    return (centred * lax.rsqrt(variance + eps_norm) * norm_gain[None, :]).astype(jnp.bfloat16)


def mixing_weights(expert_scores, group_prob):
    shifted = expert_scores - jnp.max(expert_scores, axis=1, keepdims=True)
    exp_scores = jnp.exp(shifted)
    return exp_scores / jnp.sum(exp_scores, axis=1, keepdims=True) * group_prob[:, None]


def expert_rows(flat_rows, gate_matrix, up_matrix, down_matrix):
    gate_act = jnp.dot(flat_rows, gate_matrix, preferred_element_type=jnp.float32)
    up_act = jnp.dot(flat_rows, up_matrix, preferred_element_type=jnp.float32)
    hidden = (jax.nn.silu(gate_act) * up_act).astype(jnp.bfloat16)
    return jnp.dot(hidden, down_matrix, preferred_element_type=jnp.float32).astype(jnp.bfloat16)


def local(
    tokens, norm_gain, expert_ids, expert_scores, group_prob, gate_weight, up_weight, down_weight
):
    normed = layer_norm(tokens, norm_gain)
    weights_tok = mixing_weights(expert_scores, group_prob)
    expert_count = lax.axis_size("ep")
    expert_iota = jnp.arange(expert_count, dtype=jnp.int32)
    matches = expert_ids[:, :, None] == expert_iota[None, None, :]
    route_weight = jnp.sum(jnp.where(matches, weights_tok[:, :, None], 0.0), axis=1)
    rows = lax.all_gather(normed, "ep", axis=0, tiled=True)
    own_weight = lax.all_to_all(route_weight.T, "ep", split_axis=0, concat_axis=0, tiled=True)
    results = expert_rows(rows, gate_weight[0], up_weight[0], down_weight[0])
    scaled = (results.astype(jnp.float32) * own_weight.reshape(-1)[:, None]).astype(jnp.bfloat16)
    return lax.psum_scatter(scaled, "ep", scatter_dimension=0, tiled=True)


def solution(mesh):
    in_specs = (
        P("ep", None),
        P(),
        P("ep", None),
        P("ep", None),
        P("ep"),
        P("ep", None, None),
        P("ep", None, None),
        P("ep", None, None),
    )
    out_specs = P("ep", None)
    return jax.shard_map(local, mesh=mesh, in_specs=in_specs, out_specs=out_specs, check_vma=False)
```

```python
import functools

import jax
import jax.numpy as jnp
from jax import lax
from jax.experimental import pallas as pl
from jax.experimental.pallas import tpu as pltpu
from jax.sharding import PartitionSpec as P

GROUPS = 4
TOP_K = 4
LANES = 128
MESH = pl.DeviceIdType.MESH


eps_norm = 1e-05


def layer_norm(tokens, norm_gain):
    values = tokens.astype(jnp.float32)
    average = jnp.mean(values, axis=1, keepdims=True)
    centred = values - average
    variance = jnp.mean(centred * centred, axis=1, keepdims=True)
    return (centred * lax.rsqrt(variance + eps_norm) * norm_gain[None, :]).astype(jnp.bfloat16)


def mixing_weights(expert_scores, group_prob):
    shifted = expert_scores - jnp.max(expert_scores, axis=1, keepdims=True)
    exp_scores = jnp.exp(shifted)
    return exp_scores / jnp.sum(exp_scores, axis=1, keepdims=True) * group_prob[:, None]


def expert_rows(flat_rows, gate_matrix, up_matrix, down_matrix):
    gate_act = jnp.dot(flat_rows, gate_matrix, preferred_element_type=jnp.float32)
    up_act = jnp.dot(flat_rows, up_matrix, preferred_element_type=jnp.float32)
    hidden = (jax.nn.silu(gate_act) * up_act).astype(jnp.bfloat16)
    return jnp.dot(hidden, down_matrix, preferred_element_type=jnp.float32).astype(jnp.bfloat16)


def local(
    tokens, norm_gain, expert_ids, expert_scores, group_prob, gate_weight, up_weight, down_weight
):
    normed = layer_norm(tokens, norm_gain)
    weights_tok = mixing_weights(expert_scores, group_prob)
    tok_count = tokens.shape[0]
    model_width = tokens.shape[1]
    expert_count = lax.axis_size("ep")
    group_size = expert_count // GROUPS
    capacity = (tok_count * TOP_K + group_size - 1) // group_size
    expert_iota = jnp.arange(expert_count, dtype=jnp.int32)
    slot_iota = jnp.arange(capacity, dtype=jnp.int32)
    matches = expert_ids[:, :, None] == expert_iota[None, None, :]
    route_weight = jnp.sum(jnp.where(matches, weights_tok[:, :, None], 0.0), axis=1)
    gate_matrix = gate_weight[0]
    up_matrix = up_weight[0]
    down_matrix = down_weight[0]
    chosen = jnp.sum(matches.astype(jnp.int32), axis=1)
    order_rank = jnp.cumsum(chosen, axis=0) - chosen
    slot_map = (chosen.T[:, None, :] == 1) & (order_rank.T[:, None, :] == slot_iota[None, :, None])
    outgoing = jnp.einsum(
        "emt,td->emd", slot_map.astype(jnp.bfloat16), normed, preferred_element_type=jnp.float32
    ).astype(jnp.bfloat16)
    received = lax.all_to_all(outgoing, "ep", split_axis=0, concat_axis=0, tiled=True)
    flat_rows = received.reshape(-1, model_width)
    results = expert_rows(flat_rows, gate_matrix, up_matrix, down_matrix).reshape(received.shape)
    returned_rows = lax.all_to_all(results, "ep", split_axis=0, concat_axis=0, tiled=True)
    slot_scale = jnp.where(slot_map, route_weight.T[:, None, :], 0.0)
    mixture = jnp.einsum(
        "emt,emd->td",
        slot_scale,
        returned_rows.astype(jnp.float32),
        precision=lax.Precision.HIGHEST,
    )
    return mixture.astype(jnp.bfloat16)

def ring_kernel(
    zs, tok_ref, gain_ref, ids_ref, score_ref, prob_ref, gate_hbm, up_hbm, down_hbm, out_ref,
    x0, x1, p0, p1, rd0, rd1, rb0, rb1, ra0, ra1, rz0, rz1, wg, wu, wd, w_sem,
    gather_recv, gather_pair_recv, gather_z, gather_x, gather_y, gather_pair,
    pair_recv, pair_send, far_recv, far_send, near_recv, near_send, line_recv, line_send,
):
    xs, ps, rds, rbs, ras, rzs = (x0, x1), (p0, p1), (rd0, rd1), (rb0, rb1), (ra0, ra1), (rz0, rz1)
    me = lax.axis_index("ep")
    core = lax.rem(me, 2)
    x = lax.rem(lax.div(me, 2), 2)
    y = lax.rem(lax.div(me, 4), 2)
    z = lax.div(me, 8)

    def device(zz, yy, xx, cc):
        return ((zz * 2 + yy) * 2 + xx) * 2 + cc

    partner = device(z, y, x, 1 - core)
    x_side = device(z, y, 1 - x, core)
    y_side = device(z, 1 - y, x, core)
    z_side = (device(z - 1, y, x, core), device(z + 1, y, x, core))
    has = (z > 0, z < zs - 1)
    chunks = [yy * 2 + xx for yy in (y, 1 - y) for xx in (x, 1 - x)]

    def base(rel, cc):
        return (chunks[rel] * 2 + cc) * zs

    copies = [
        pltpu.make_async_copy(src.at[0], dst, w_sem.at[i])
        for i, (src, dst) in enumerate(((gate_hbm, wg), (up_hbm, wu), (down_hbm, wd)))
    ]
    for copy in copies:
        copy.start()

    barrier = pltpu.get_barrier_semaphore()
    for other in (partner, x_side, y_side):
        pl.semaphore_signal(barrier, inc=1, device_id=(other,), device_id_type=MESH)
    for d in (0, 1):
        @pl.when(has[d])
        def _():
            pl.semaphore_signal(barrier, inc=1, device_id=(z_side[d],), device_id_type=MESH)

    model_width = tok_ref.shape[1]
    half = x0.shape[2]
    values = tok_ref[...].astype(jnp.float32)
    average = jnp.sum(values, axis=1, keepdims=True) * (1.0 / model_width)
    centred = values - average
    variance = jnp.sum(centred * centred, axis=1, keepdims=True) * (1.0 / model_width)
    normed = (centred * lax.rsqrt(variance + eps_norm) * gain_ref[...]).astype(jnp.bfloat16)
    score = [score_ref[:, k : k + 1] for k in range(TOP_K)]
    top = functools.reduce(jnp.maximum, score)
    exps = [jnp.exp(s - top) for s in score]
    total = functools.reduce(jnp.add, exps)
    lane = lax.broadcasted_iota(jnp.int32, (tok_ref.shape[0], LANES), 1)
    meta = jnp.zeros((tok_ref.shape[0], LANES), jnp.float32)
    for k in range(TOP_K):
        weight = exps[k] / total * prob_ref[...]
        high = weight.astype(jnp.bfloat16).astype(jnp.float32)
        meta = jnp.where(lane == k, ids_ref[:, k : k + 1].astype(jnp.float32), meta)
        meta = jnp.where(lane == TOP_K + k, high, meta)
        meta = jnp.where(lane == 2 * TOP_K + k, weight - high, meta)
    own = base(0, core) + z
    x0[own] = normed[:, :half]
    x1[own, :, : model_width - half] = normed[:, half:]
    x1[own, :, model_width - half :] = meta.astype(jnp.bfloat16)

    inside = jnp.logical_and(has[0], has[1])

    @pl.when(inside)
    def _():
        pl.semaphore_wait(barrier, 5)

    @pl.when(jnp.logical_not(inside))
    def _():
        pl.semaphore_wait(barrier, 4)

    pending = []

    def send(src, dst, send_sem, recv_sem, target, conds=()):
        array, index = send_sem
        pltpu.make_async_remote_copy(
            src_ref=src(), dst_ref=dst(), send_sem=array.at[index], recv_sem=recv_sem,
            device_id=(target,), device_id_type=MESH,
        ).start()

        def finish():
            sem = array.at[index]
            pltpu.make_async_remote_copy(
                src_ref=src(), dst_ref=dst(), send_sem=sem, recv_sem=sem,
                device_id=(target,), device_id_type=MESH,
            ).wait_send()

        pending.append((conds, finish))

    def landed(dst, recv_sem):
        pltpu.make_async_remote_copy(
            src_ref=dst, dst_ref=dst, send_sem=recv_sem, recv_sem=recv_sem,
            device_id=(partner,), device_id_type=MESH,
        ).wait_recv()

    def at_distance(s, body):
        if s == 0:
            body(z, (), None)
            return
        for d, q, ok in ((1, z - s, z - s >= 0), (0, z + s, z + s < zs)):
            @pl.when(ok)
            def _():
                body(q, (ok,), d)

    def spread(q, conds, came):
        for h in (0, 1):
            block = functools.partial(lambda h: xs[h].at[base(0, core) + q], h)
            if came is not None:
                landed(block(), gather_recv.at[h, 0, q])
            for d in (0, 1):
                if came is None or came == d:
                    @pl.when(has[d])
                    def _():
                        send(block, block, (gather_z, (h, d, q)), gather_recv.at[h, 0, q],
                             z_side[d], conds + (has[d],))
            send(block, block, (gather_x, (h, 0, q)), gather_recv.at[h, 1, q], x_side, conds)
            send(block, block, (gather_y, (h, 0, q)), gather_recv.at[h, 2, q], y_side, conds)

    def forward(q, conds, _):
        block = lambda: x0.at[base(1, core) + q]
        landed(block(), gather_recv.at[0, 1, q])
        send(block, block, (gather_y, (0, 1, q)), gather_recv.at[0, 3, q], y_side, conds)
        other = lambda: x1.at[base(2, core) + q]
        landed(other(), gather_recv.at[1, 2, q])
        send(other, other, (gather_x, (1, 1, q)), gather_recv.at[1, 3, q], x_side, conds)

    def all_landed(h, rel):
        for q in range(zs):
            landed(xs[h].at[base(rel, core) + q], gather_recv.at[h, rel, q])

    def pair_gather(rel):
        for h in (0, 1):
            blocks = functools.partial(lambda h: xs[h].at[pl.ds(base(rel, core), zs)], h)
            send(blocks, blocks, (gather_pair, (h, rel)), gather_pair_recv.at[h, rel], partner)

    def compute(rel):
        for h in (0, 1):
            landed(xs[h].at[pl.ds(base(rel, 1 - core), zs)], gather_pair_recv.at[h, rel])
        slots = pl.ds(chunks[rel] * 2 * zs, 2 * zs)
        rows = 2 * zs * tok_ref.shape[0]
        left = x0[slots].reshape(rows, half)
        right = x1[slots, :, : model_width - half].reshape(rows, model_width - half)
        tags = x1[slots, :, model_width - half :].reshape(rows, LANES).astype(jnp.float32)
        expert = me.astype(jnp.float32)
        scale = jnp.zeros((rows, 1), jnp.float32)
        for k in range(TOP_K):
            value = tags[:, TOP_K + k : TOP_K + k + 1] + tags[:, 2 * TOP_K + k : 2 * TOP_K + k + 1]
            scale += jnp.where(tags[:, k : k + 1] == expert, value, 0.0)

        def project(w):
            return jnp.dot(left, w[:half, :], preferred_element_type=jnp.float32) + jnp.dot(
                right, w[half:, :], preferred_element_type=jnp.float32
            )

        gate_act = project(wg)
        up_act = project(wu)
        hidden = (jax.nn.silu(gate_act) * up_act).astype(jnp.bfloat16)
        step = half // 3 if half % (3 * LANES) == 0 else half
        for h in (0, 1):
            width = ps[h].shape[2]
            for at in range(0, width, step):
                part = jnp.dot(hidden, wd[:, h * half + at : h * half + at + step],
                               preferred_element_type=jnp.float32)
                part = (part.astype(jnp.bfloat16).astype(jnp.float32) * scale).astype(jnp.bfloat16)
                ps[h][slots, :, at : at + step] = part.reshape(2 * zs, tok_ref.shape[0], step)

    def pair_reduce(rel):
        for h in (0, 1):
            part = functools.partial(lambda h: ps[h].at[pl.ds(base(rel, 1 - core), zs)], h)
            room = functools.partial(lambda h: rds[h].at[rel], h)
            send(part, room, (pair_send, (h, rel)), pair_recv.at[h, rel], partner)

    def pair_add(rel):
        for h in (0, 1):
            landed(rds[h].at[rel], pair_recv.at[h, rel])
            slots = pl.ds(base(rel, core), zs)
            ps[h][slots] = ps[h][slots] + rds[h][rel]

    far_side = (y_side, x_side)
    near_side = (x_side, y_side)

    def far(h, rel, kind):
        def body(q, conds, _):
            send(lambda: ps[h].at[base(rel, core) + q], lambda: rbs[h].at[kind, q],
                 (far_send, (h, kind, q)), far_recv.at[h, kind, q], far_side[h], conds)
        return body

    def near(q, conds, _):
        for h in (0, 1):
            landed(rbs[h].at[1, q], far_recv.at[h, 1, q])
            slot = base(1 + h, core) + q
            ps[h][slot] = ps[h][slot] + rbs[h][1, q]
            part = functools.partial(lambda h: ps[h].at[base(1 + h, core) + q], h)
            room = functools.partial(lambda h: ras[h].at[q], h)
            send(part, room, (near_send, (h, q)), near_recv.at[h, q],
                 near_side[h], conds)

    def line(q, conds, d):
        for h in (0, 1):
            landed(rbs[h].at[0, q], far_recv.at[h, 0, q])
            landed(ras[h].at[q], near_recv.at[h, q])
            slot = base(0, core) + q
            held = ps[h][slot].astype(jnp.float32) + rbs[h][0, q].astype(jnp.float32)
            ps[h][slot] = (held + ras[h][q].astype(jnp.float32)).astype(jnp.bfloat16)
            if d is None:
                for side in (0, 1):
                    @pl.when(has[side])
                    def _():
                        landed(rzs[h].at[side, q], line_recv.at[h, side, q])
                        ps[h][slot] = ps[h][slot] + rzs[h][side, q]
                width = ps[h].shape[2]
                out_ref[:, h * half : h * half + width] = ps[h][slot]
            else:
                @pl.when(has[d])
                def _():
                    landed(rzs[h].at[d, q], line_recv.at[h, d, q])
                    ps[h][slot] = ps[h][slot] + rzs[h][d, q]
                part = functools.partial(lambda h: ps[h].at[base(0, core) + q], h)
                room = functools.partial(lambda h: rzs[h].at[d, q], h)
                send(part, room, (line_send, (h, d, q)),
                     line_recv.at[h, d, q], z_side[1 - d], conds)

    def far_first(body):
        for s in range(zs - 1, -1, -1):
            at_distance(s, body)

    at_distance(0, spread)
    for s in range(1, zs):
        at_distance(s, spread)
        at_distance(s - 1, forward)
    pair_gather(0)
    for copy in copies:
        copy.wait()
    compute(0)
    pair_reduce(0)
    at_distance(zs - 1, forward)
    all_landed(1, 1)
    pair_gather(1)
    all_landed(0, 2)
    pair_gather(2)
    compute(1)
    pair_reduce(1)
    compute(2)
    pair_reduce(2)
    pair_add(1)
    far_first(far(1, 1, 0))
    pair_add(2)
    far_first(far(0, 2, 0))
    for h in (0, 1):
        all_landed(h, 3)
    pair_gather(3)
    compute(3)
    pair_reduce(3)
    pair_add(0)
    pair_add(3)
    far_first(far(0, 3, 1))
    far_first(far(1, 3, 1))
    at_distance(zs - 1, near)
    for s in range(zs - 2, -1, -1):
        at_distance(s, near)
        at_distance(s + 1, line)
    at_distance(0, line)

    for conds, finish in pending:
        if conds:
            pl.when(functools.reduce(jnp.logical_and, conds))(finish)
        else:
            finish()


def ring_local(
    zs, tokens, norm_gain, expert_ids, expert_scores, group_prob, gate_weight, up_weight, down_weight
):
    count, width = tokens.shape
    hidden = gate_weight.shape[2]
    slots = zs * 8
    half = width // 2
    kind = jnp.bfloat16
    vmem = pl.BlockSpec(memory_space=pltpu.VMEM)
    hbm = pl.BlockSpec(memory_space=pl.ANY)
    dma = pltpu.SemaphoreType.DMA
    widths = (half, width - half)
    each = lambda *lead: [pltpu.VMEM(lead + (count, w), kind) for w in widths]
    scratch = [
        pltpu.VMEM((slots, count, half), kind),
        pltpu.VMEM((slots, count, width - half + LANES), kind),
        *each(slots), *each(4, zs), *each(2, zs), *each(zs), *each(2, zs),
        pltpu.VMEM((width, hidden), kind), pltpu.VMEM((width, hidden), kind),
        pltpu.VMEM((hidden, width), kind), dma((3,)),
        dma((2, 4, zs)), dma((2, 4)), dma((2, 2, zs)), dma((2, 2, zs)), dma((2, 2, zs)), dma((2, 4)),
        dma((2, 4)), dma((2, 4)), dma((2, 2, zs)), dma((2, 2, zs)),
        dma((2, zs)), dma((2, zs)), dma((2, 2, zs)), dma((2, 2, zs)),
    ]
    return pl.pallas_call(
        functools.partial(ring_kernel, zs),
        out_shape=jax.ShapeDtypeStruct((count, width), kind),
        in_specs=[vmem] * 5 + [hbm] * 3,
        out_specs=vmem,
        scratch_shapes=scratch,
        compiler_params=pltpu.CompilerParams(
            collective_id=0, has_side_effects=True, vmem_limit_bytes=60 * 1024 * 1024
        ),
    )(
        tokens, norm_gain[None, :], expert_ids, expert_scores, group_prob[:, None],
        gate_weight, up_weight, down_weight,
    )


def solution(mesh):
    in_specs = (
        P("ep", None),
        P(),
        P("ep", None),
        P("ep", None),
        P("ep"),
        P("ep", None, None),
        P("ep", None, None),
        P("ep", None, None),
    )
    out_specs = P("ep", None)
    devices = mesh.shape["ep"]
    body = functools.partial(ring_local, GROUPS) if devices == GROUPS * 8 else local
    return jax.shard_map(body, mesh=mesh, in_specs=in_specs, out_specs=out_specs, check_vma=False)
```

```python
import functools

import jax
import jax.numpy as jnp
from jax import lax
from jax.experimental import pallas as pl
from jax.experimental.pallas import tpu as pltpu
from jax.sharding import PartitionSpec as P

GROUPS = 4
TOP_K = 4
LANES = 128
MESH = pl.DeviceIdType.MESH


eps_norm = 1e-05


def layer_norm(tokens, norm_gain):
    values = tokens.astype(jnp.float32)
    average = jnp.mean(values, axis=1, keepdims=True)
    centred = values - average
    variance = jnp.mean(centred * centred, axis=1, keepdims=True)
    return (centred * lax.rsqrt(variance + eps_norm) * norm_gain[None, :]).astype(jnp.bfloat16)


def mixing_weights(expert_scores, group_prob):
    shifted = expert_scores - jnp.max(expert_scores, axis=1, keepdims=True)
    exp_scores = jnp.exp(shifted)
    return exp_scores / jnp.sum(exp_scores, axis=1, keepdims=True) * group_prob[:, None]


def expert_rows(flat_rows, gate_matrix, up_matrix, down_matrix):
    gate_act = jnp.dot(flat_rows, gate_matrix, preferred_element_type=jnp.float32)
    up_act = jnp.dot(flat_rows, up_matrix, preferred_element_type=jnp.float32)
    hidden = (jax.nn.silu(gate_act) * up_act).astype(jnp.bfloat16)
    return jnp.dot(hidden, down_matrix, preferred_element_type=jnp.float32).astype(jnp.bfloat16)


def local(
    tokens, norm_gain, expert_ids, expert_scores, group_prob, gate_weight, up_weight, down_weight
):
    normed = layer_norm(tokens, norm_gain)
    weights_tok = mixing_weights(expert_scores, group_prob)
    tok_count = tokens.shape[0]
    model_width = tokens.shape[1]
    expert_count = lax.axis_size("ep")
    group_size = expert_count // GROUPS
    capacity = (tok_count * TOP_K + group_size - 1) // group_size
    expert_iota = jnp.arange(expert_count, dtype=jnp.int32)
    slot_iota = jnp.arange(capacity, dtype=jnp.int32)
    matches = expert_ids[:, :, None] == expert_iota[None, None, :]
    route_weight = jnp.sum(jnp.where(matches, weights_tok[:, :, None], 0.0), axis=1)
    gate_matrix = gate_weight[0]
    up_matrix = up_weight[0]
    down_matrix = down_weight[0]
    chosen = jnp.sum(matches.astype(jnp.int32), axis=1)
    order_rank = jnp.cumsum(chosen, axis=0) - chosen
    slot_map = (chosen.T[:, None, :] == 1) & (order_rank.T[:, None, :] == slot_iota[None, :, None])
    outgoing = jnp.einsum(
        "emt,td->emd", slot_map.astype(jnp.bfloat16), normed, preferred_element_type=jnp.float32
    ).astype(jnp.bfloat16)
    received = lax.all_to_all(outgoing, "ep", split_axis=0, concat_axis=0, tiled=True)
    flat_rows = received.reshape(-1, model_width)
    results = expert_rows(flat_rows, gate_matrix, up_matrix, down_matrix).reshape(received.shape)
    returned_rows = lax.all_to_all(results, "ep", split_axis=0, concat_axis=0, tiled=True)
    slot_scale = jnp.where(slot_map, route_weight.T[:, None, :], 0.0)
    mixture = jnp.einsum(
        "emt,emd->td",
        slot_scale,
        returned_rows.astype(jnp.float32),
        precision=lax.Precision.HIGHEST,
    )
    return mixture.astype(jnp.bfloat16)

def ring_kernel(
    zs, tok_ref, gain_ref, ids_ref, score_ref, prob_ref, gate_hbm, up_hbm, down_hbm, out_ref,
    x0, x1, p0, p1, rd0, rd1, rb0, rb1, ra0, ra1, rz0, rz1, wg, wu, wd, w_sem,
    gather_recv, gather_pair_recv, gather_z, gather_x, gather_y, gather_pair,
    pair_recv, pair_send, far_recv, far_send, near_recv, near_send, line_recv, line_send,
):
    xs, ps, rds, rbs, ras, rzs = (x0, x1), (p0, p1), (rd0, rd1), (rb0, rb1), (ra0, ra1), (rz0, rz1)
    me = lax.axis_index("ep")
    core = lax.rem(me, 2)
    x = lax.rem(lax.div(me, 2), 2)
    y = lax.rem(lax.div(me, 4), 2)
    z = lax.div(me, 8)

    def device(zz, yy, xx, cc):
        return ((zz * 2 + yy) * 2 + xx) * 2 + cc

    partner = device(z, y, x, 1 - core)
    x_side = device(z, y, 1 - x, core)
    y_side = device(z, 1 - y, x, core)
    z_side = (device(z - 1, y, x, core), device(z + 1, y, x, core))
    has = (z > 0, z < zs - 1)
    chunks = [yy * 2 + xx for yy in (y, 1 - y) for xx in (x, 1 - x)]

    def base(rel, cc):
        return (chunks[rel] * 2 + cc) * zs

    copies = [
        pltpu.make_async_copy(src.at[0], dst, w_sem.at[i])
        for i, (src, dst) in enumerate(((gate_hbm, wg), (up_hbm, wu), (down_hbm, wd)))
    ]
    for copy in copies:
        copy.start()

    barrier = pltpu.get_barrier_semaphore()
    for other in (partner, x_side, y_side):
        pl.semaphore_signal(barrier, inc=1, device_id=(other,), device_id_type=MESH)
    for d in (0, 1):
        @pl.when(has[d])
        def _():
            pl.semaphore_signal(barrier, inc=1, device_id=(z_side[d],), device_id_type=MESH)

    model_width = tok_ref.shape[1]
    half = x0.shape[2]
    values = tok_ref[...].astype(jnp.float32)
    average = jnp.sum(values, axis=1, keepdims=True) * (1.0 / model_width)
    centred = values - average
    variance = jnp.sum(centred * centred, axis=1, keepdims=True) * (1.0 / model_width)
    normed = (centred * lax.rsqrt(variance + eps_norm) * gain_ref[...]).astype(jnp.bfloat16)
    count = tok_ref.shape[0]
    score = [score_ref[k : k + 1, :] for k in range(TOP_K)]
    top = functools.reduce(jnp.maximum, score)
    exps = [jnp.exp(s - top) for s in score]
    total = functools.reduce(jnp.add, exps)
    row = lax.broadcasted_iota(jnp.int32, (LANES, count), 0)
    tags = jnp.zeros((LANES, count), jnp.float32)
    for k in range(TOP_K):
        weight = exps[k] / total * prob_ref[...]
        high = weight.astype(jnp.bfloat16).astype(jnp.float32)
        tags = jnp.where(row == k, ids_ref[k : k + 1, :].astype(jnp.float32), tags)
        tags = jnp.where(row == TOP_K + k, high, tags)
        tags = jnp.where(row == 2 * TOP_K + k, weight - high, tags)
    square = (count, count)
    same = lax.broadcasted_iota(jnp.int32, square, 0) == lax.broadcasted_iota(jnp.int32, square, 1)
    meta = lax.dot_general(
        same.astype(jnp.float32).astype(jnp.bfloat16), tags.astype(jnp.bfloat16),
        (((1,), (1,)), ((), ())), preferred_element_type=jnp.float32,
    )
    own = base(0, core) + z
    x0[own] = normed[:, :half]
    x1[own, :, : model_width - half] = normed[:, half:]
    x1[own, :, model_width - half :] = meta.astype(jnp.bfloat16)

    inside = jnp.logical_and(has[0], has[1])

    @pl.when(inside)
    def _():
        pl.semaphore_wait(barrier, 5)

    @pl.when(jnp.logical_not(inside))
    def _():
        pl.semaphore_wait(barrier, 4)

    pending = []

    def send(src, dst, send_sem, recv_sem, target, conds=()):
        array, index = send_sem
        pltpu.make_async_remote_copy(
            src_ref=src(), dst_ref=dst(), send_sem=array.at[index], recv_sem=recv_sem,
            device_id=(target,), device_id_type=MESH,
        ).start()

        def finish():
            sem = array.at[index]
            pltpu.make_async_remote_copy(
                src_ref=src(), dst_ref=dst(), send_sem=sem, recv_sem=sem,
                device_id=(target,), device_id_type=MESH,
            ).wait_send()

        pending.append((conds, finish))

    def landed(dst, recv_sem):
        pltpu.make_async_remote_copy(
            src_ref=dst, dst_ref=dst, send_sem=recv_sem, recv_sem=recv_sem,
            device_id=(partner,), device_id_type=MESH,
        ).wait_recv()

    def at_distance(s, body):
        if s == 0:
            body(z, (), None)
            return
        for d, q, ok in ((1, z - s, z - s >= 0), (0, z + s, z + s < zs)):
            @pl.when(ok)
            def _():
                body(q, (ok,), d)

    def spread(q, conds, came):
        for h in (0, 1):
            block = functools.partial(lambda h: xs[h].at[base(0, core) + q], h)
            if came is not None:
                landed(block(), gather_recv.at[h, 0, q])
            for d in (0, 1):
                if came is None or came == d:
                    @pl.when(has[d])
                    def _():
                        send(block, block, (gather_z, (h, d, q)), gather_recv.at[h, 0, q],
                             z_side[d], conds + (has[d],))
            send(block, block, (gather_x, (h, 0, q)), gather_recv.at[h, 1, q], x_side, conds)
            send(block, block, (gather_y, (h, 0, q)), gather_recv.at[h, 2, q], y_side, conds)

    def forward(q, conds, _):
        block = lambda: x0.at[base(1, core) + q]
        landed(block(), gather_recv.at[0, 1, q])
        send(block, block, (gather_y, (0, 1, q)), gather_recv.at[0, 3, q], y_side, conds)
        other = lambda: x1.at[base(2, core) + q]
        landed(other(), gather_recv.at[1, 2, q])
        send(other, other, (gather_x, (1, 1, q)), gather_recv.at[1, 3, q], x_side, conds)

    def all_landed(h, rel):
        for q in range(zs):
            landed(xs[h].at[base(rel, core) + q], gather_recv.at[h, rel, q])

    def pair_gather(rel):
        for h in (0, 1):
            blocks = functools.partial(lambda h: xs[h].at[pl.ds(base(rel, core), zs)], h)
            send(blocks, blocks, (gather_pair, (h, rel)), gather_pair_recv.at[h, rel], partner)

    def compute(rel):
        for h in (0, 1):
            landed(xs[h].at[pl.ds(base(rel, 1 - core), zs)], gather_pair_recv.at[h, rel])
        slots = pl.ds(chunks[rel] * 2 * zs, 2 * zs)
        rows = 2 * zs * tok_ref.shape[0]
        left = x0[slots].reshape(rows, half)
        right = x1[slots, :, : model_width - half].reshape(rows, model_width - half)
        tags = x1[slots, :, model_width - half :].reshape(rows, LANES).astype(jnp.float32)
        expert = me.astype(jnp.float32)
        scale = jnp.zeros((rows, 1), jnp.float32)
        for k in range(TOP_K):
            value = tags[:, TOP_K + k : TOP_K + k + 1] + tags[:, 2 * TOP_K + k : 2 * TOP_K + k + 1]
            scale += jnp.where(tags[:, k : k + 1] == expert, value, 0.0)

        def project(w):
            return jnp.dot(left, w[:half, :], preferred_element_type=jnp.float32) + jnp.dot(
                right, w[half:, :], preferred_element_type=jnp.float32
            )

        gate_act = project(wg)
        up_act = project(wu)
        hidden = (jax.nn.silu(gate_act) * up_act).astype(jnp.bfloat16)
        step = half // 3 if half % (3 * LANES) == 0 else half
        for h in (0, 1):
            width = ps[h].shape[2]
            for at in range(0, width, step):
                part = jnp.dot(hidden, wd[:, h * half + at : h * half + at + step],
                               preferred_element_type=jnp.float32)
                part = (part.astype(jnp.bfloat16).astype(jnp.float32) * scale).astype(jnp.bfloat16)
                ps[h][slots, :, at : at + step] = part.reshape(2 * zs, tok_ref.shape[0], step)

    def pair_reduce(rel):
        for h in (0, 1):
            part = functools.partial(lambda h: ps[h].at[pl.ds(base(rel, 1 - core), zs)], h)
            room = functools.partial(lambda h: rds[h].at[rel], h)
            send(part, room, (pair_send, (h, rel)), pair_recv.at[h, rel], partner)

    def pair_add(rel):
        for h in (0, 1):
            landed(rds[h].at[rel], pair_recv.at[h, rel])
            slots = pl.ds(base(rel, core), zs)
            ps[h][slots] = ps[h][slots] + rds[h][rel]

    far_side = (y_side, x_side)
    near_side = (x_side, y_side)

    def far(h, rel, kind):
        def body(q, conds, _):
            send(lambda: ps[h].at[base(rel, core) + q], lambda: rbs[h].at[kind, q],
                 (far_send, (h, kind, q)), far_recv.at[h, kind, q], far_side[h], conds)
        return body

    def near(q, conds, _):
        for h in (0, 1):
            landed(rbs[h].at[1, q], far_recv.at[h, 1, q])
            slot = base(1 + h, core) + q
            ps[h][slot] = ps[h][slot] + rbs[h][1, q]
            part = functools.partial(lambda h: ps[h].at[base(1 + h, core) + q], h)
            room = functools.partial(lambda h: ras[h].at[q], h)
            send(part, room, (near_send, (h, q)), near_recv.at[h, q],
                 near_side[h], conds)

    def line(q, conds, d):
        for h in (0, 1):
            landed(rbs[h].at[0, q], far_recv.at[h, 0, q])
            landed(ras[h].at[q], near_recv.at[h, q])
            slot = base(0, core) + q
            held = ps[h][slot].astype(jnp.float32) + rbs[h][0, q].astype(jnp.float32)
            ps[h][slot] = (held + ras[h][q].astype(jnp.float32)).astype(jnp.bfloat16)
            if d is None:
                for side in (0, 1):
                    @pl.when(has[side])
                    def _():
                        landed(rzs[h].at[side, q], line_recv.at[h, side, q])
                        ps[h][slot] = ps[h][slot] + rzs[h][side, q]
                width = ps[h].shape[2]
                out_ref[:, h * half : h * half + width] = ps[h][slot]
            else:
                @pl.when(has[d])
                def _():
                    landed(rzs[h].at[d, q], line_recv.at[h, d, q])
                    ps[h][slot] = ps[h][slot] + rzs[h][d, q]
                part = functools.partial(lambda h: ps[h].at[base(0, core) + q], h)
                room = functools.partial(lambda h: rzs[h].at[d, q], h)
                send(part, room, (line_send, (h, d, q)),
                     line_recv.at[h, d, q], z_side[1 - d], conds)

    def far_first(body):
        for s in range(zs - 1, -1, -1):
            at_distance(s, body)

    at_distance(0, spread)
    for s in range(1, zs):
        at_distance(s, spread)
        at_distance(s - 1, forward)
    pair_gather(0)
    for copy in copies:
        copy.wait()
    compute(0)
    pair_reduce(0)
    at_distance(zs - 1, forward)
    all_landed(1, 1)
    pair_gather(1)
    all_landed(0, 2)
    pair_gather(2)
    compute(1)
    pair_reduce(1)
    pair_add(1)
    far_first(far(1, 1, 0))
    compute(2)
    pair_reduce(2)
    pair_add(0)
    pair_add(2)
    far_first(far(0, 2, 0))
    for h in (0, 1):
        all_landed(h, 3)
    pair_gather(3)
    compute(3)
    pair_reduce(3)
    pair_add(3)
    far_first(far(0, 3, 1))
    far_first(far(1, 3, 1))
    at_distance(zs - 1, near)
    for s in range(zs - 2, -1, -1):
        at_distance(s, near)
        at_distance(s + 1, line)
    at_distance(0, line)

    for conds, finish in pending:
        if conds:
            pl.when(functools.reduce(jnp.logical_and, conds))(finish)
        else:
            finish()


def ring_local(
    zs, tokens, norm_gain, expert_ids, expert_scores, group_prob, gate_weight, up_weight, down_weight
):
    count, width = tokens.shape
    hidden = gate_weight.shape[2]
    slots = zs * 8
    half = width // 2
    kind = jnp.bfloat16
    vmem = pl.BlockSpec(memory_space=pltpu.VMEM)
    hbm = pl.BlockSpec(memory_space=pl.ANY)
    dma = pltpu.SemaphoreType.DMA
    widths = (half, width - half)
    each = lambda *lead: [pltpu.VMEM(lead + (count, w), kind) for w in widths]
    scratch = [
        pltpu.VMEM((slots, count, half), kind),
        pltpu.VMEM((slots, count, width - half + LANES), kind),
        *each(slots), *each(4, zs), *each(2, zs), *each(zs), *each(2, zs),
        pltpu.VMEM((width, hidden), kind), pltpu.VMEM((width, hidden), kind),
        pltpu.VMEM((hidden, width), kind), dma((3,)),
        dma((2, 4, zs)), dma((2, 4)), dma((2, 2, zs)), dma((2, 2, zs)), dma((2, 2, zs)), dma((2, 4)),
        dma((2, 4)), dma((2, 4)), dma((2, 2, zs)), dma((2, 2, zs)),
        dma((2, zs)), dma((2, zs)), dma((2, 2, zs)), dma((2, 2, zs)),
    ]
    return pl.pallas_call(
        functools.partial(ring_kernel, zs),
        out_shape=jax.ShapeDtypeStruct((count, width), kind),
        in_specs=[vmem] * 5 + [hbm] * 3,
        out_specs=vmem,
        scratch_shapes=scratch,
        compiler_params=pltpu.CompilerParams(
            collective_id=0, has_side_effects=True, vmem_limit_bytes=60 * 1024 * 1024
        ),
    )(
        tokens, norm_gain[None, :], expert_ids.T, expert_scores.T, group_prob[None, :], gate_weight, up_weight, down_weight,
    )


def solution(mesh):
    in_specs = (
        P("ep", None),
        P(),
        P("ep", None),
        P("ep", None),
        P("ep"),
        P("ep", None, None),
        P("ep", None, None),
        P("ep", None, None),
    )
    out_specs = P("ep", None)
    devices = mesh.shape["ep"]
    body = functools.partial(ring_local, GROUPS) if devices == GROUPS * 8 else local
    return jax.shard_map(body, mesh=mesh, in_specs=in_specs, out_specs=out_specs, check_vma=False)
```
